768 devices in a mesh: ep: 48 (over z, x), tp: 16 (over y, core).
Axes of the slice: x: 4, y: 8, z: 12, core: 2. Of those that a mesh axis runs over, the one named last changes fastest.
Arguments:
- tokens: bfloat16 [9216, 2048], P('ep'), may hold values from -6 to 6
- cotangent: bfloat16 [9216, 2048], P('ep'), may hold values from -6 to 6
- routing: int32 [9216, 2], P('ep'), may hold values from 0 to 47, all different within a row; in each aligned block of 192 rows (0 to 191, 192 to 383, ...) at most 10 rows name the same one
- route_weights: float32 [9216, 2], P('ep'), may hold values from 0.1 to 1
- w_gate: bfloat16 [48, 2048, 2048], P('ep', None, 'tp'), may hold values from -0.125 to 0.125
- w_up: bfloat16 [48, 2048, 2048], P('ep', None, 'tp'), may hold values from -0.125 to 0.125
- w_down: bfloat16 [48, 2048, 2048], P('ep', 'tp'), may hold values from -0.125 to 0.125
Outputs:
- grad_tokens: bfloat16 [9216, 2048], P('ep')
- grad_weights: bfloat16 [9216, 2], P('ep')
- grad_gate: bfloat16 [48, 2048, 2048], P('ep', None, 'tp')
- grad_up: bfloat16 [48, 2048, 2048], P('ep', None, 'tp')
- grad_down: bfloat16 [48, 2048, 2048], P('ep', 'tp')
The draws below stay inside these ranges and needn't reach their ends.
Inputs may be any that keep to these rules, and one draw needn't show every extreme that they name: `routing`: each row names 2 different experts. Within the rows of one device no expert is named more than 10 times, and in every draw some expert is named exactly 10 times by some device's rows.
All inputs are finite; a program needn't handle non-finite values.
Results may differ from the reference program's by a relative error of at most 0.019.
Values may be sent and summed in bfloat16 or wider, within the bound.
A program may use at most 64 MiB of HBM per device.

```python
import math
import jax
import jax.numpy as jnp
import numpy as np
from jax import lax

D = 2048
F = 2048
TOP = 2
TOK_DEV = 192
EXPERTS = 48
CAP = 10
TOKENS = 9216
N_EP = 48
N_TP = 16


def levels(stream_key, dims, cuts, least, top_value):
    gain, own = 1.0, jax.random.fold_in(stream_key, 6)
    for axis_at, blocks in cuts:
        draws = jnp.exp(jax.random.uniform(jax.random.fold_in(own, axis_at), (blocks,), jnp.float32, least / len(cuts), top_value / len(cuts)))
        gain = gain * jnp.repeat(draws, dims[axis_at] // blocks).reshape([-1 if axis == axis_at else 1 for axis in range(len(dims))])
    return gain


def deal_out(key, own, number, rows, amount, top, most, lean):
    ranking = jax.random.permutation(key, amount)
    packed, ordinary = portions_of(amount, rows * top, most, lean, True), portions_of(amount, rows * top, most, lean, False)
    places = jnp.arange(amount)

    def named(lengths, turn):
        used = int((lengths > 0).sum())
        fixed = max(1, used // 4)
        shifted = fixed + (places - fixed + turn * (used - fixed)) % max(1, amount - fixed)
        return jnp.zeros((amount,), jnp.int32).at[ranking[jnp.where(places < fixed, places, shifted)]].set(jnp.asarray(lengths, jnp.int32))

    lengths = jnp.where(number % 4 == 0, named(packed, number // 4), named(ordinary, number - number // 4 - 1))
    mixed = jax.random.permutation(jax.random.fold_in(own, 3), amount)
    donor, sink = mixed[0:amount // 2 * 2:2], mixed[1:amount // 2 * 2:2]
    room = jnp.minimum(lengths[donor] - 1, most - lengths[sink]) // 2
    room = jnp.where((donor == ranking[0]) | (sink == ranking[0]) | (lengths[sink] == 0), 0, jnp.maximum(room, 0))
    shifted = jax.random.randint(jax.random.fold_in(own, 4), (amount // 2,), 0, 1 << 20) % (room + 1)
    lengths = lengths.at[donor].add(-shifted).at[sink].add(shifted)
    members = jnp.searchsorted(jnp.cumsum(lengths), jnp.arange(rows * top), side="right").astype(jnp.int32)
    grid = members.reshape(top, rows).T
    grid = grid[jax.random.permutation(jax.random.fold_in(own, 1), rows)]
    turn = jax.random.randint(jax.random.fold_in(own, 2), (rows, 1), 0, top)
    return jnp.take_along_axis(grid, (jnp.arange(top)[None, :] + turn) % top, axis=1)


def portions_of(count, total, most, lean, full):
    loads = [(1 << 20) // math.isqrt(grade ** lean) + 1 for grade in range(1, count + 1)]
    largest = most if full else min(most, max(-(-total // count), total * loads[0] // sum(loads)))
    least = 1 if total - largest >= count - 1 else 0
    holding, surplus = [largest] + [least] * (count - 1), total - largest - least * (count - 1)
    while surplus > 0:
        candidates = [i for i in range(1, count) if holding[i] < largest] or [i for i in range(1, count) if holding[i] < most]
        pool, remaining = sum([loads[i] for i in candidates]), surplus
        for i in candidates:
            more = min(most - holding[i], max(1, remaining * loads[i] // pool), surplus)
            holding[i] = holding[i] + more
            surplus = surplus - more
    return np.array(holding)


def noise(key, extent, spread, most, cuts=(), kind=jnp.bfloat16):
    factor_of = levels(key, extent, cuts, -0.22, 0.18) if cuts else 1.0
    drawn = jax.random.normal(key, extent, jnp.float32) * spread * factor_of
    return jnp.minimum(jnp.maximum(drawn, -most), most).astype(kind)


def setup_inputs(seed: int = 0) -> dict:
    keys = jax.random.split(jax.random.key(seed), 8)
    tokens = noise(keys[0], (TOKENS, D), 1.0, 6.0, ((0, 48),))
    cotangent = noise(keys[1], (TOKENS, D), 1.0, 6.0, ((0, 48),))
    routing_keys = jax.random.split(jax.random.fold_in(keys[2], 1), TOKENS // TOK_DEV)
    routing_turns = jax.random.permutation(jax.random.fold_in(keys[2], 3), TOKENS // TOK_DEV)
    routing = jax.vmap(lambda own, number: deal_out(jax.random.fold_in(keys[2], 2), own, number, TOK_DEV, EXPERTS, TOP, CAP, 2))(routing_keys, routing_turns).reshape((TOKENS, TOP))
    route_weights = jnp.clip(jnp.exp(math.log(1.0) - 2.3025851 * jax.random.uniform(keys[3], (TOKENS, TOP), jnp.float32) ** levels(keys[3], (TOKENS, TOP), ((0, 48),), -0.2, 0.2)), 0.1, 1.0)
    w_gate = noise(keys[4], (EXPERTS, D, F), D ** -0.5, 0.125, ((0, 48), (2, 16)))
    w_up = noise(keys[5], (EXPERTS, D, F), D ** -0.5, 0.125, ((0, 48), (2, 16)))
    w_down = noise(keys[6], (EXPERTS, F, D), F ** -0.5, 0.125, ((0, 48), (1, 16)))
    return {"tokens": tokens, "cotangent": cotangent, "routing": routing, "route_weights": route_weights, "w_gate": w_gate, "w_up": w_up, "w_down": w_down}


def reference(tokens, cotangent, routing, route_weights, w_gate, w_up, w_down):
    all_tokens = tokens.shape[0]
    experts = EXPERTS
    blocks = routing.reshape(N_EP, TOK_DEV * TOP)
    onehot = (blocks[:, :, None] == jnp.arange(experts, dtype=jnp.int32)[None, None, :]).astype(jnp.int32)
    before = jnp.cumsum(onehot, axis=1) - onehot
    within = jnp.sum(before * onehot, axis=2)
    source = jnp.arange(N_EP, dtype=jnp.int32)[:, None]
    place = (source * CAP + within).reshape(-1).astype(jnp.int32)
    expert_of = routing.reshape(-1).astype(jnp.int32)
    token_of = jnp.repeat(jnp.arange(all_tokens, dtype=jnp.int32), TOP)
    slot_count = N_EP * CAP
    table = jnp.full((experts, slot_count), all_tokens, jnp.int32).at[expert_of, place].set(token_of)
    rounded = lax.optimization_barrier(route_weights.astype(jnp.bfloat16)).astype(jnp.float32).reshape(-1)
    weight_table = jnp.zeros((experts, slot_count), jnp.float32).at[expert_of, place].set(rounded)
    padded_rows = jnp.concatenate([tokens, jnp.zeros((1, D), jnp.bfloat16)], 0)
    padded_back = jnp.concatenate([cotangent, jnp.zeros((1, D), jnp.bfloat16)], 0)
    hidden_block = F // N_TP

    def one_expert(args):
        index, weight, wgate, wup, wdown = args
        rows = padded_rows[index]
        back = padded_back[index]
        weight = weight[:, None]
        pre_gate = jnp.dot(rows, wgate, preferred_element_type=jnp.float32)
        pre_up = jnp.dot(rows, wup, preferred_element_type=jnp.float32)
        along = jnp.dot(back, wdown.T, preferred_element_type=jnp.float32)
        gate_sig = jax.nn.sigmoid(pre_gate)
        gate_act = pre_gate * gate_sig
        hidden = gate_act * pre_up
        hidden_grad = weight * along
        gate_grad = (hidden_grad * pre_up * gate_sig * (1.0 + pre_gate * (1.0 - gate_sig))).astype(jnp.bfloat16)
        up_grad = (hidden_grad * gate_act).astype(jnp.bfloat16)
        scaled = (weight * hidden).astype(jnp.bfloat16)
        grad_gate = jnp.dot(rows.T, gate_grad, preferred_element_type=jnp.float32).astype(jnp.bfloat16)
        grad_up = jnp.dot(rows.T, up_grad, preferred_element_type=jnp.float32).astype(jnp.bfloat16)
        grad_down = jnp.dot(scaled.T, back, preferred_element_type=jnp.float32).astype(jnp.bfloat16)
        slot_total = index.shape[0]
        gate_blocks = gate_grad.astype(jnp.float32).reshape(slot_total, N_TP, hidden_block)
        up_blocks = up_grad.astype(jnp.float32).reshape(slot_total, N_TP, hidden_block)
        wgate_blocks = wgate.astype(jnp.float32).reshape(D, N_TP, hidden_block)
        wup_blocks = wup.astype(jnp.float32).reshape(D, N_TP, hidden_block)
        row_part = jnp.einsum('rbf,dbf->rbd', gate_blocks, wgate_blocks) + jnp.einsum('rbf,dbf->rbd', up_blocks, wup_blocks)
        row_part = lax.optimization_barrier(row_part.astype(jnp.bfloat16)).astype(jnp.float32)
        slot_rows = jnp.sum(row_part, axis=1).astype(jnp.bfloat16)
        slot_part = jnp.sum((hidden * along).reshape(slot_total, N_TP, hidden_block), axis=2)
        slot_part = lax.optimization_barrier(slot_part.astype(jnp.bfloat16)).astype(jnp.float32)
        slot_grad = jnp.sum(slot_part, axis=1).astype(jnp.bfloat16)
        return slot_rows, slot_grad, grad_gate, grad_up, grad_down

    slot_rows, slot_grad, grad_gate, grad_up, grad_down = lax.map(
        one_expert, (table, weight_table, w_gate, w_up, w_down))
    picked = slot_rows[expert_of, place].astype(jnp.float32).reshape(all_tokens, TOP, D)
    grad_tokens = jnp.sum(picked, axis=1).astype(jnp.bfloat16)
    grad_weights = slot_grad[expert_of, place].reshape(all_tokens, TOP)
    return grad_tokens, grad_weights, grad_gate, grad_up, grad_down
```

```python
import functools

import jax
import jax.numpy as jnp
from jax import lax
from jax.experimental import pallas as pl
from jax.experimental.pallas import tpu as pltpu
from jax.sharding import PartitionSpec as P

MESH = pl.DeviceIdType.MESH
BF = jnp.bfloat16
F32 = jnp.float32
CAP = 10
MSG = 24
RET = 16
NN = (((1,), (0,)), ((), ()))
NT = (((1,), (1,)), ((), ()))
TN = (((0,), (0,)), ((), ()))


def dot(a, b, dims=NN):
    return lax.dot_general(a, b, dims, preferred_element_type=F32)


def iota(shape, dim):
    return lax.broadcasted_iota(jnp.int32, shape, dim)


def remote(src, dst, send, recv, device):
    return pltpu.make_async_remote_copy(
        src_ref=src, dst_ref=dst, send_sem=send, recv_sem=recv,
        device_id=device, device_id_type=MESH)


def kernel(n_ep, n_tp, tok_h, cot_h, wg_h, wu_h, wd_h, rt, rtT, rwT,
           out, gw, ggate, gup, gdown,
           tok, cot, W, WD, WDT, WT, WTP, SO, SI, G, GG, GP, SC, SPR, TP, DS, DR, SM, RB, TM,
           in_sem, a_send, a_recv, w_sem, b_send, b_recv, m_send, m_recv, g_send, g_recv,
           d_send, d_recv, e_send, e_recv, f_send, f_recv, fm_send, fm_recv):
    ny = n_tp // 2
    nx = ny // 2
    nz = n_ep // nx
    km = n_ep // n_tp
    xbits = nx.bit_length() - 1
    width = tok.shape[1]
    half_w = width // 2
    ntok = tok.shape[0]
    hid = WD.shape[0]
    slots = n_tp * 32

    e = lax.axis_index("ep")
    t = lax.axis_index("tp")
    z, x = lax.div(e, nx), lax.rem(e, nx)
    y, c = lax.div(t, 2), lax.rem(t, 2)

    def at_y(step):
        return lax.rem(y + (step % ny), ny)

    def dev_y(step):
        return {"tp": at_y(step) * 2 + c}

    def dev_e(dz, dx):
        return {"ep": lax.rem(z + nz + dz, nz) * nx + lax.rem(x + nx + dx, nx)}

    mate = {"tp": y * 2 + 1 - c}

    loads = [
        pltpu.make_async_copy(tok_h, tok, in_sem.at[0]),
        pltpu.make_async_copy(cot_h, cot, in_sem.at[1]),
        pltpu.make_async_copy(wg_h, W.at[:, pl.ds(0, hid)], in_sem.at[2]),
        pltpu.make_async_copy(wu_h, W.at[:, pl.ds(hid, hid)], in_sem.at[3]),
        pltpu.make_async_copy(wd_h, WD, in_sem.at[4]),
    ]
    for copy in loads:
        copy.start()

    barrier = pltpu.get_barrier_semaphore()

    def greet(d, carry):
        pl.semaphore_signal(barrier, inc=1, device_id=dev_e(lax.div(d, nx), lax.rem(d, nx)), device_id_type=MESH)
        return carry

    lax.fori_loop(1, n_ep, greet, 0)
    for device in (dev_y(1), dev_y(-1), mate):
        pl.semaphore_signal(barrier, inc=1, device_id=device, device_id_type=MESH)
    others = n_ep - 1 + 3
    for step in range(2, ny - 1):
        pl.semaphore_signal(barrier, inc=1, device_id=dev_y(step), device_id_type=MESH)
        others += 1

    dz0 = 2 * c + lax.rem(y, 2)
    dx0 = lax.div(y, 2)
    rows = km * MSG
    ri = iota((rows, ntok), 0)
    kk = jnp.zeros((rows, ntok), jnp.int32)
    for k in range(1, km):
        kk = kk + (ri >= k * MSG).astype(jnp.int32)
    s_in = ri - kk * MSG
    ex = lax.rem(x + dx0, nx)
    want = jnp.zeros((rows, ntok), jnp.int32)
    for k in range(km):
        expert_k = lax.rem(z + dz0 + 4 * k, nz) * nx + ex
        want = jnp.where(kk == k, expert_k, want)
    hit0 = rtT[0:1, :] == want
    hit1 = rtT[1:2, :] == want
    hit = jnp.where(hit0 | hit1, 1.0, 0.0)
    before = jnp.where(iota((ntok, ntok), 0) < iota((ntok, ntok), 1), 1.0, 0.0).astype(BF)
    rank = dot(hit.astype(BF), before).astype(jnp.int32)
    q_tok = jnp.where(rank == s_in, hit, 0.0)
    q_cot = jnp.where(rank + CAP == s_in, hit, 0.0)
    q_cot = jnp.where(s_in >= CAP, q_cot, 0.0)
    q_cot = jnp.where(s_in < 2 * CAP, q_cot, 0.0)
    q_tok = jnp.where(s_in < CAP, q_tok, 0.0)
    w_hit = jnp.where(hit0, rwT[0:1, :], rwT[1:2, :]).astype(BF).astype(F32)
    w_col = jnp.sum(q_tok * w_hit, axis=1, keepdims=True)
    li = iota((rows, 128), 1)
    ri1 = iota((rows, 128), 0)
    kk1 = jnp.zeros((rows, 128), jnp.int32)
    for k in range(1, km):
        kk1 = kk1 + (ri1 >= k * MSG).astype(jnp.int32)
    s1 = ri1 - kk1 * MSG
    w_diag = jnp.where((li == kk1 * CAP + s1) & (s1 < CAP), w_col, 0.0).astype(BF)
    rr, rc = iota((rows, rows), 0), iota((rows, rows), 1)
    collect = jnp.zeros((rows, rows), F32)
    for k in range(km):
        collect = jnp.where((rr == k * MSG + 2 * CAP) & (rc >= k * MSG) & (rc < k * MSG + MSG), 1.0, collect)
    w_rows = dot(collect.astype(BF), w_diag)
    q_tok = q_tok.astype(BF)
    q_cot = q_cot.astype(BF)
    loads[0].wait()
    loads[1].wait()
    tile = min(512, width)
    for j in range(width // tile):
        cols = slice(j * tile, (j + 1) * tile)
        part = dot(q_tok, tok[:, cols]) + dot(q_cot, cot[:, cols])
        SO[:, cols] = part.astype(BF)
        if j == 0:
            SO[:, 0:128] = (part[:, 0:128] + w_rows).astype(BF)

    pl.semaphore_wait(barrier, others)

    def a_copy(k):
        return remote(SO.at[pl.ds(k * MSG, MSG)], SI.at[pl.ds(k * MSG, MSG)], a_send.at[k], a_recv.at[k],
                      dev_e(dz0 + 4 * k, dx0))

    order = [k for k in range(km) if k == 1] + [k for k in range(km) if k != 1]
    for k in order:
        if k == 0:
            @pl.when(t != 0)
            def _():
                a_copy(0).start()

            @pl.when(t == 0)
            def _():
                SI[0:MSG, :] = SO[0:MSG, :]
        else:
            a_copy(k).start()

    for copy in loads[2:]:
        copy.wait()
    for j in range(n_tp):
        WT[j % 2, j // 2] = W[j * 128:(j + 1) * 128, :].T
        WDT[j * 128:(j + 1) * 128, :] = WD[:, j * 128:(j + 1) * 128].T
    w_copy = remote(WT.at[1 - c], WTP, w_sem.at[0], w_sem.at[1], mate)
    w_copy.start()

    lane = iota((ntok, 128), 1)
    r0, r1 = rt[:, 0:1], rt[:, 1:2]

    def entry_places():
        h0, h1 = r0 == lane, r1 == lane
        named = jnp.where(h0 | h1, 1.0, 0.0).astype(BF)
        lower = jnp.where(iota((ntok, ntok), 1) < iota((ntok, ntok), 0), 1.0, 0.0).astype(BF)
        count = dot(lower, named)
        n0 = jnp.sum(jnp.where(h0, count, 0.0), axis=1, keepdims=True).astype(jnp.int32)
        n1 = jnp.sum(jnp.where(h1, count, 0.0), axis=1, keepdims=True).astype(jnp.int32)

        def place(r, n):
            dz = (r >> xbits) - z
            dz = jnp.where(dz < 0, dz + nz, dz)
            dx = ((r & (nx - 1)) + nx - x) & (nx - 1)
            group = 4 * dx + 2 * (dz & 1) + ((dz >> 1) & 1)
            k = dz >> 2
            return (group * km + k) * RET, (group & 3) * 32 + k * CAP + n

        m0, l0 = place(r0, n0)
        m1, l1 = place(r1, n1)
        return m0, n0, l0, m1, n1, l1

    m0, n0, _, m1, n1, _ = entry_places()
    for j in range(n_ep * RET // 128):
        col = lane + 128 * j
        TM[:, j * 128:(j + 1) * 128] = jnp.where((col == m0 + n0) | (col == m1 + n1), 1.0, 0.0).astype(BF)

    pr, pc = iota((64, rows), 0), iota((64, rows), 1)
    pack = jnp.zeros((64, rows), F32)
    for k in range(km):
        lo = k * CAP
        pack = jnp.where((pr >= lo) & (pr < lo + CAP) & (pc == pr - lo + k * MSG), 1.0, pack)
        pack = jnp.where((pr == 30) & (pc == k * MSG + 2 * CAP), 1.0, pack)
        pack = jnp.where((pr >= 32 + lo) & (pr < 32 + lo + CAP) & (pc == pr - 32 - lo + k * MSG + CAP), 1.0, pack)
    pack = pack.astype(BF)
    for k in order:
        if k == 0:
            @pl.when(t != 0)
            def _():
                a_copy(0).wait()
        else:
            a_copy(k).wait()
    mine = pl.ds(pl.multiple_of(t * 32, 32), 32)
    htile = min(512, half_w)
    for j in range(width // htile):
        part = dot(pack, SI[:, j * htile:(j + 1) * htile]).astype(BF)
        h, off = (j * htile) // half_w, (j * htile) % half_w
        G[0, h, mine, off:off + htile] = part[0:32]
        G[1, h, mine, off:off + htile] = part[32:64]

    long_hops, short_hops = ny // 2, ny // 2 - 1
    flows = [(1, 0, long_hops), (-1, 1, long_hops), (1, 1, short_hops), (-1, 0, short_hops)]
    pieces = {}
    for sgn, h, hops in flows:
        for s in range(1, hops + 1):
            pieces[(sgn, h, s)] = len(pieces)

    def piece(h, yo):
        return G.at[:, h, pl.ds(pl.multiple_of((yo * 2 + c) * 32, 32), 32), :]

    def ring(sgn, h, s):
        i = pieces[(sgn, h, s)]
        yo = at_y(-sgn * (s - 1))
        return remote(piece(h, yo), piece(h, yo), b_send.at[i], b_recv.at[i], dev_y(sgn))

    def share(i, h, yo):
        return remote(piece(h, yo), piece(h, yo), m_send.at[i], m_recv.at[i], mate)

    for sgn, h, hops in flows:
        ring(sgn, h, 1).start()
    for h in range(2):
        share(len(pieces) + h, h, y).start()

    def expert(yo, sem):
        here = pl.ds(pl.multiple_of(yo * 64, 64), 64)
        ra, rb = G[0, 0, here, :], G[0, 1, here, :]
        pre = dot(ra, W[0:half_w, :]) + dot(rb, W[half_w:, :])
        along = dot(G[1, 0, here, :], WDT[0:half_w, :]) + dot(G[1, 1, here, :], WDT[half_w:, :])
        pre_gate, pre_up = pre[:, 0:hid], pre[:, hid:]
        wf = ra[:, 0:128].astype(F32)
        row, col = iota((64, 128), 0), iota((64, 128), 1)
        wf = jnp.where(row < 32, wf[30:31, :], wf[62:63, :])
        weight = jnp.sum(jnp.where((row & 31) == col, wf, 0.0), axis=1, keepdims=True)
        sig = jax.nn.sigmoid(pre_gate)
        act = pre_gate * sig
        hidden = act * pre_up
        hidden_grad = weight * along
        gate_grad = hidden_grad * pre_up * sig * (1.0 + pre_gate * (1.0 - sig))
        GG[here, 0:hid] = gate_grad.astype(BF)
        GG[here, hid:2 * hid] = (hidden_grad * act).astype(BF)
        part = jnp.sum(hidden * along, axis=1, keepdims=True)
        GG[here, 2 * hid:3 * hid] = jnp.broadcast_to(part, (64, hid)).astype(BF)
        SC[here, :] = (weight * hidden).astype(BF)
        grads(yo, sem).start()

    def grads(yo, sem):
        here = pl.ds(pl.multiple_of(yo * 64, 64), 64)
        return remote(GG.at[here], GP.at[here], g_send.at[sem], g_recv.at[sem], mate)

    for h in range(2):
        share(len(pieces) + h, h, y).wait_recv()
    expert(y, 0)
    for s in range(1, long_hops + 1):
        for sgn, h, hops in flows:
            if s <= hops:
                i = pieces[(sgn, h, s)]
                yo = at_y(-sgn * s)
                remote(piece(h, yo), piece(h, yo), b_send.at[i], b_recv.at[i], dev_y(sgn)).wait_recv()
                if s < hops:
                    ring(sgn, h, s + 1).start()
                share(i, h, yo).start()
        for sgn, h, hops in flows:
            if s <= hops:
                share(pieces[(sgn, h, s)], h, at_y(-sgn * s)).wait_recv()
        expert(at_y(-s), s)
        if s < long_hops:
            expert(at_y(s), ny - s)

    w_copy.wait()
    grads(y, 0).wait()
    for s in range(1, long_hops + 1):
        grads(at_y(-s), s).wait()
        if s < long_hops:
            grads(at_y(s), ny - s).wait()

    nq = 4
    quarter = slots // nq

    def row_part(j):
        yt = at_y(j)
        for p in range(2):
            cut = slice(p * slots // 2, (p + 1) * slots // 2)
            TP[j % ny, cut, :] = dot(GG[cut, 0:2 * hid], WT[c, yt]) + dot(GP[cut, 0:2 * hid], WTP[yt])

    row_part(long_hops)
    for q in range(nq):
        cut = slice(q * quarter, (q + 1) * quarter)
        both = GG[cut, 2 * hid:3 * hid].astype(F32) + GP[cut, 2 * hid:3 * hid].astype(F32)
        diag = jnp.where(iota((quarter, 128), 0) == iota((quarter, 128), 1), both[:, 0:128], 0.0)
        SPR[q] = jnp.broadcast_to(jnp.sum(diag, axis=0, keepdims=True), (8, 128))

    def hops_of(sgn, q):
        return long_hops if (sgn > 0) == (q < nq // 2) else short_hops

    parts = {}
    for sgn in (1, -1):
        for q in range(nq):
            for s in range(1, hops_of(sgn, q) + 1):
                parts[(sgn, q, s)] = len(parts)

    def d_copy(sgn, q, s):
        i = parts[(sgn, q, s)]
        return remote(DS.at[i], DR.at[i], d_send.at[i], d_recv.at[i], dev_y(sgn))

    def hop(sgn, q, s):
        i = parts[(sgn, q, s)]
        target = sgn * (hops_of(sgn, q) + 1 - s)
        val = TP[target % ny, q * quarter:(q + 1) * quarter, :]
        slot = SPR[q]
        if s > 1:
            d_copy(sgn, q, s - 1).wait_recv()
            j = parts[(sgn, q, s - 1)]
            val = val + DR[j, 0:quarter, :].astype(F32)
            slot = slot + DR[j, quarter:, :].astype(F32)
        DS[i, 0:quarter, :] = val.astype(BF)
        DS[i, quarter:, :] = slot.astype(BF)
        d_copy(sgn, q, s).start()

    low, high = range(nq // 2), range(nq // 2, nq)
    for q in range(nq // 2):
        hop(1, q, 1)
        hop(-1, q + nq // 2, 1)
    row_part(short_hops)
    for q in high:
        hop(1, q, 1)
    row_part(-short_hops)
    for q in low:
        hop(-1, q, 1)
    for s in range(2, long_hops + 1):
        if short_hops + 1 - s >= 0:
            row_part(short_hops + 1 - s)
            if short_hops + 1 - s > 0:
                row_part(-(short_hops + 1 - s))
        for q in range(nq // 2):
            hop(1, q, s)
            hop(-1, q + nq // 2, s)
        if s <= short_hops:
            for q in range(nq // 2):
                hop(1, q + nq // 2, s)
                hop(-1, q, s)

    e_rows = slots // nq // 32 * km * RET
    ur, uc = iota((e_rows, quarter + 8), 0), iota((e_rows, quarter + 8), 1)
    unpack = jnp.zeros((e_rows, quarter + 8), F32)
    for m in range(e_rows // RET):
        base = (m // km) * 32 + (m % km) * CAP
        lo = m * RET
        unpack = jnp.where((ur >= lo) & (ur < lo + CAP) & (uc == ur - lo + base), 1.0, unpack)
        unpack = jnp.where((ur == lo + CAP) & (uc == quarter), 1.0, unpack)
    unpack = unpack.astype(BF)
    per_q = e_rows // RET
    for q in range(nq):
        val = TP[0, q * quarter:(q + 1) * quarter, :]
        slot = SPR[q]
        for sgn in (1, -1):
            last = hops_of(sgn, q)
            d_copy(sgn, q, last).wait_recv()
            j = parts[(sgn, q, last)]
            val = val + DR[j, 0:quarter, :].astype(F32)
            slot = slot + DR[j, quarter:, :].astype(F32)
        total = jnp.concatenate([val, slot], axis=0).astype(BF)
        messages = dot(unpack, total).astype(BF)
        SM[q * e_rows:(q + 1) * e_rows, :] = messages
        if q == 0:
            RB[0:RET, :] = messages[0:RET]
        for m in range(per_q):
            i = q * per_q + m
            if i == 0:
                continue
            group, k = i // km, i % km
            dx, rem = group // 4, group % 4
            dz = 4 * k + 2 * (rem % 2) + rem // 2
            place = pl.ds(i * RET, RET)
            remote(SM.at[place], RB.at[place], e_send, e_recv, dev_e(-dz, -dx)).start()

    for h in range(2):
        for j in range(half_w // 256):
            cols = slice(j * 256, (j + 1) * 256)
            there = slice(h * half_w + j * 256, h * half_w + (j + 1) * 256)
            both = dot(G[0, h, :, cols], GG[:, 0:2 * hid], TN)
            ggate[there, :] = both[:, 0:hid].astype(BF)
            gup[there, :] = both[:, hid:].astype(BF)
            gdown[:, there] = dot(SC[...], G[1, h, :, cols], TN).astype(BF)

    rest = pl.ds(RET, (n_ep - 1) * RET)
    home = remote(SM.at[rest], RB.at[rest], e_send, e_recv, mate)
    home.wait_recv()

    def features(step, same=True):
        to = at_y(step) * 2 + c
        return out.at[:, pl.ds(pl.multiple_of(to * 128, 128), 128)]

    out[:, pl.ds(pl.multiple_of(t * 128, 128), 128)] = dot(TM[...], RB[...]).astype(BF)

    def f_copy(i, step):
        return remote(features(0), features(0), f_send.at[i], f_recv.at[i], dev_y(step))

    far_first = sorted(range(1, ny), key=lambda s: -min(s, ny - s))
    for i, step in enumerate(far_first):
        f_copy(i, step).start()

    def pass_on(i, step):
        return remote(features(step), features(step), fm_send.at[i], fm_recv.at[i], mate)

    pass_on(ny - 1, 0).start()

    m0, n0, l0, m1, n1, l1 = entry_places()
    got0 = jnp.zeros((ntok, 128), F32)
    got1 = jnp.zeros((ntok, 128), F32)
    for j in range(n_ep * RET // 128):
        col = lane + 128 * j
        there = RB[j * 128:(j + 1) * 128, :]
        got0 = got0 + dot(jnp.where(col == m0 + CAP, 1.0, 0.0).astype(BF), there)
        got1 = got1 + dot(jnp.where(col == m1 + CAP, 1.0, 0.0).astype(BF), there)
    w0 = jnp.sum(jnp.where(lane == l0, got0, 0.0), axis=1, keepdims=True)
    w1 = jnp.sum(jnp.where(lane == l1, got1, 0.0), axis=1, keepdims=True)
    gw[...] = jnp.where(iota((ntok, 2), 1) == 0, w0, w1).astype(BF)

    near_first = sorted(range(1, ny), key=lambda s: min(s, ny - s))
    for step in near_first:
        i = far_first.index(step)
        back = far_first.index((-step) % ny)
        remote(features(step), features(step), f_send.at[back], f_recv.at[back], dev_y(-step)).wait_recv()
        pass_on(i, step).start()
    pass_on(ny - 1, 0).wait_recv()
    for step in near_first:
        pass_on(far_first.index(step), step).wait_recv()

    for (sgn, h, s), i in pieces.items():
        ring(sgn, h, s).wait_send()
        share(i, h, at_y(-sgn * s)).wait_send()
    for h in range(2):
        share(len(pieces) + h, h, y).wait_send()
    for key in parts:
        d_copy(*key).wait_send()
    home.wait_send()
    for i, step in enumerate(far_first):
        f_copy(i, step).wait_send()
        pass_on(i, step).wait_send()
    pass_on(ny - 1, 0).wait_send()


def on_device(n_ep, n_tp, tokens, cotangent, routing, route_weights, w_gate, w_up, w_down):
    ntok, width = tokens.shape
    hid = w_gate.shape[2]
    ny = n_tp // 2
    km = n_ep // n_tp
    slots = n_tp * 32
    pieces = 2 * (ny - 1)
    parts = 4 * (ny - 1)
    vmem = pl.BlockSpec(memory_space=pltpu.VMEM)
    hbm = pl.BlockSpec(memory_space=pl.ANY)
    dma = pltpu.SemaphoreType.DMA
    grad_tokens, grad_weights, grad_gate, grad_up, grad_down = pl.pallas_call(
        functools.partial(kernel, n_ep, n_tp),
        out_shape=(
            jax.ShapeDtypeStruct((ntok, width), BF),
            jax.ShapeDtypeStruct((ntok, 2), BF),
            jax.ShapeDtypeStruct((width, hid), BF),
            jax.ShapeDtypeStruct((width, hid), BF),
            jax.ShapeDtypeStruct((hid, width), BF),
        ),
        in_specs=[hbm] * 5 + [vmem] * 3,
        out_specs=[vmem] * 5,
        scratch_shapes=[
            pltpu.VMEM((ntok, width), BF),
            pltpu.VMEM((ntok, width), BF),
            pltpu.VMEM((width, 2 * hid), BF),
            pltpu.VMEM((hid, width), BF),
            pltpu.VMEM((width, hid), BF),
            pltpu.VMEM((2, ny, 2 * hid, 128), BF),
            pltpu.VMEM((ny, 2 * hid, 128), BF),
            pltpu.VMEM((km * MSG, width), BF),
            pltpu.VMEM((km * MSG, width), BF),
            pltpu.VMEM((2, 2, slots, width // 2), BF),
            pltpu.VMEM((slots, 3 * hid), BF),
            pltpu.VMEM((slots, 3 * hid), BF),
            pltpu.VMEM((slots, hid), BF),
            pltpu.VMEM((4, 8, 128), F32),
            pltpu.VMEM((ny, slots, 128), F32),
            pltpu.VMEM((parts, slots // 4 + 8, 128), BF),
            pltpu.VMEM((parts, slots // 4 + 8, 128), BF),
            pltpu.VMEM((n_ep * RET, 128), BF),
            pltpu.VMEM((n_ep * RET, 128), BF),
            pltpu.VMEM((ntok, n_ep * RET), BF),
            dma((5,)),
            dma((km,)), dma((km,)),
            dma((2,)),
            dma((pieces,)), dma((pieces,)),
            dma((pieces + 2,)), dma((pieces + 2,)),
            dma((ny,)), dma((ny,)),
            dma((parts,)), dma((parts,)),
            dma, dma,
            dma((ny - 1,)), dma((ny - 1,)),
            dma((ny,)), dma((ny,)),
        ],
        compiler_params=pltpu.CompilerParams(
            collective_id=0, has_side_effects=True, vmem_limit_bytes=56 * 1024 * 1024),
    )(tokens, cotangent, w_gate[0], w_up[0], w_down[0], routing, routing.T, route_weights.T)
    return (grad_tokens, grad_weights, grad_gate[None], grad_up[None], grad_down[None])


def solution(mesh):
    n_ep, n_tp = mesh.shape["ep"], mesh.shape["tp"]
    return jax.shard_map(
        functools.partial(on_device, n_ep, n_tp),
        mesh=mesh,
        in_specs=(
            P("ep", None),
            P("ep", None),
            P("ep", None),
            P("ep", None),
            P("ep", None, "tp"),
            P("ep", None, "tp"),
            P("ep", "tp", None),
        ),
        out_specs=(
            P("ep", None),
            P("ep", None),
            P("ep", None, "tp"),
            P("ep", None, "tp"),
            P("ep", "tp", None),
        ),
        check_vma=False,
    )
```
